32 devices in a mesh: grp: 2 (over y), ep: 4 (over z), tp: 4 (over x, core).
Axes of the slice: x: 2, y: 2, z: 4, core: 2. Of those that a mesh axis runs over, the one named last changes fastest.
Arguments:
- mixer_input: bfloat16 [4096, 2048], P(('grp', 'ep', 'tp')), parts along dimension 0, may hold values from -8 to 8
- forget_cumsum: float32 [8, 4096], P('tp', 'grp'), parts along dimension 1, may hold values from -259 to 0, as said below
- mixer_gain: float32 [2048], replicated, may hold values from 0.1 to 1.9
- query_weight: bfloat16 [2048, 1024], P(None, 'tp'), may hold values from -6 to 6
- key_weight: bfloat16 [2048, 1024], P(None, 'tp'), may hold values from -6 to 6
- value_weight: bfloat16 [2048, 1024], P(None, 'tp'), may hold values from -0.125 to 0.125
- out_weight: bfloat16 [1024, 2048], P('tp'), may hold values from -0.1875 to 0.1875
- post_gain: float32 [2048], replicated, may hold values from 0.1 to 1.9
- expert_input: bfloat16 [4096, 2048], P(('grp', 'ep', 'tp')), parts along dimension 0, may hold values from -6 to 6
- expert_gain: float32 [2048], replicated, may hold values from 0.1 to 1.9
- routes: int32 [4096, 2], P(('grp', 'ep', 'tp')), parts along dimension 0, may hold values from 0 to 3, all different within a row; in each aligned block of 128 rows (0 to 127, 128 to 255, ...) at most 72 rows name the same one
- route_weight: float32 [4096, 2], P(('grp', 'ep', 'tp')), parts along dimension 0, may hold values from 0.2 to 1
- expert_gate: bfloat16 [4, 2048, 2048], P('ep', None, 'tp'), may hold values from -0.125 to 0.125
- expert_upward: bfloat16 [4, 2048, 2048], P('ep', None, 'tp'), may hold values from -0.125 to 0.125
- expert_down: bfloat16 [4, 2048, 2048], P('ep', 'tp'), may hold values from -0.125 to 0.125
Outputs:
- mixer_output: bfloat16 [4096, 2048], P(('grp', 'ep', 'tp')), parts along dimension 0
- expert_output: bfloat16 [4096, 2048], P(('grp', 'ep', 'tp')), parts along dimension 0
The draws below stay inside these ranges and needn't reach their ends.
There are 2 independent parts, one for each index of `grp`. The reference program is written for one: setup_inputs(seed, part) draws one part's arguments, and reference() takes and returns one part's arrays. A program takes and returns all parts, laid end to end along the dimension named above; an argument that names none is the same for every part. Nothing has to cross between parts.
Inputs may be any that keep to these rules, and one draw needn't show every extreme that they name: `forget_cumsum`: each head's row never rises along positions. `routes`: A row names 2 different experts. Within the rows of one device (aligned blocks of 128 rows) no expert is named by more than 72 rows, and in every draw some expert is named by exactly 72 rows of some block.
All inputs are finite; a program needn't handle non-finite values.
Results may differ from the reference program's by a relative error of at most 0.012.
Values may be sent and summed in bfloat16 or wider, within the bound.
A program may use at most 128 MiB of HBM per device.

```python
import math
import jax
import jax.numpy as jnp
import numpy as np
from jax import lax

D = 2048
ATTENDER_NUMBER = 8
HEAD_DIM = 128
EXP_FF = 2048
TOP = 2
MOE_ROWS = 128
SPAN = 512
WINDOW_EXTENT = 2048
TOK_MOE = 2048
EXPERTS = 4
CAP = 72
N_EP = 4
N_TP = 4


def draw_mixer_input(key, part):
    base = jnp.clip(jax.random.normal(jax.random.fold_in(key, 1), (WINDOW_EXTENT, D), jnp.float32), -6.0, 6.0)
    return base.astype(jnp.bfloat16)


def base_weight(key, number):
    normal = jax.random.normal(jax.random.fold_in(key, number), (D, ATTENDER_NUMBER * HEAD_DIM), jnp.float32)
    return jnp.clip(normal, -6.0, 6.0) * D ** (-0.5)


def draw_query_weight(key, part):
    return base_weight(key, 101).astype(jnp.bfloat16)


def draw_key_weight(key, part):
    return base_weight(key, 202).astype(jnp.bfloat16)


def draw_forget_cumsum(key, part):
    order = jax.random.permutation(jax.random.fold_in(key, 1), ATTENDER_NUMBER)
    fast_count = ATTENDER_NUMBER // 2
    rapid_route = order < fast_count
    fast_rate = jnp.exp(jax.random.uniform(jax.random.fold_in(key, 2), (ATTENDER_NUMBER,), jnp.float32, math.log(1.0 / 100.0), math.log(1.0 / 30.0)))
    slow_rate = 0.4 / WINDOW_EXTENT * jnp.exp(jax.random.uniform(jax.random.fold_in(key, 3), (ATTENDER_NUMBER,), jnp.float32, math.log(0.7), math.log(1.4)))
    rate = jnp.where(rapid_route, fast_rate, slow_rate)
    factor = jnp.exp(jax.random.uniform(jax.random.fold_in(key, 4), (ATTENDER_NUMBER, WINDOW_EXTENT // SPAN), jnp.float32, math.log(0.5), math.log(2.0)))
    factor = jnp.repeat(factor, SPAN, axis=1)
    jitter = jax.random.uniform(jax.random.fold_in(key, 5), (ATTENDER_NUMBER, WINDOW_EXTENT), jnp.float32, 0.3, 1.7)
    advance_increment = -rate[:, None] * factor * jitter
    flurry_slot = jax.random.randint(jax.random.fold_in(key, 6), (ATTENDER_NUMBER, 3), 0, WINDOW_EXTENT)
    flurry_extent = jnp.log(jax.random.uniform(jax.random.fold_in(key, 7), (ATTENDER_NUMBER, 3), jnp.float32, 0.5, 0.8))
    element_place = jnp.arange(WINDOW_EXTENT, dtype=jnp.int32)
    agreeing_tally = element_place[None, None, :] == flurry_slot[:, :, None]
    flurry_clusters = jnp.sum(jnp.where(agreeing_tally, flurry_extent[:, :, None], 0.0), axis=1)
    flurry_clusters = flurry_clusters * jnp.where(rapid_route, 0.0, 1.0)[:, None]
    return jnp.cumsum(advance_increment + flurry_clusters, axis=1)


def steps_of(key, dims, split, low, high):
    level = 1.0
    for dim, blocks in split:
        steps = jax.random.uniform(jax.random.fold_in(jax.random.fold_in(key, 6), dim), (blocks,), jnp.float32, low / len(split), high / len(split))
        level = level * jnp.repeat(jnp.exp(steps), dims[dim] // blocks).reshape((-1,) + (1,) * (len(dims) - 1 - dim))
    return level


def shared_out(key, own, number, rows, count, top, reach, skew):
    order = jax.random.permutation(key, count)
    packed, common = load_shares(count, rows * top, reach, skew, True), load_shares(count, rows * top, reach, skew, False)
    places = jnp.arange(count)

    def named(tallies, turn):
        used = int((tallies > 0).sum())
        fixed = max(1, used // 4)
        shifted = fixed + (places - fixed + turn * (used - fixed)) % max(1, count - fixed)
        return jnp.zeros((count,), jnp.int32).at[order[jnp.where(places < fixed, places, shifted)]].set(jnp.asarray(tallies, jnp.int32))

    tallies = jnp.where(number % 4 == 0, named(packed, number // 4), named(common, number - number // 4 - 1))
    mixed = jax.random.permutation(jax.random.fold_in(own, 3), count)
    donor, receiver = mixed[0:count // 2 * 2:2], mixed[1:count // 2 * 2:2]
    margin = jnp.minimum(tallies[donor] - 1, reach - tallies[receiver]) // 2
    margin = jnp.where((donor == order[0]) | (receiver == order[0]) | (tallies[receiver] == 0), 0, jnp.maximum(margin, 0))
    shifted = jax.random.randint(jax.random.fold_in(own, 4), (count // 2,), 0, 1 << 20) % (margin + 1)
    tallies = tallies.at[donor].add(-shifted).at[receiver].add(shifted)
    items = jnp.searchsorted(jnp.cumsum(tallies), jnp.arange(rows * top), side="right").astype(jnp.int32)
    listing = items.reshape(top, rows).T
    listing = listing[jax.random.permutation(jax.random.fold_in(own, 1), rows)]
    turn = jax.random.randint(jax.random.fold_in(own, 2), (rows, 1), 0, top)
    return jnp.take_along_axis(listing, (jnp.arange(top)[None, :] + turn) % top, axis=1)


def load_shares(amount, total, bound, skew, full):
    weights = [(1 << 20) // math.isqrt(standing ** skew) + 1 for standing in range(1, amount + 1)]
    largest = bound if full else min(bound, max(-(-total // amount), total * weights[0] // sum(weights)))
    least = 1 if total - largest >= amount - 1 else 0
    counts, surplus = [largest] + [least] * (amount - 1), total - largest - least * (amount - 1)
    while surplus > 0:
        movable = [i for i in range(1, amount) if counts[i] < largest] or [i for i in range(1, amount) if counts[i] < bound]
        mass, budget = sum([weights[i] for i in movable]), surplus
        for i in movable:
            addition = min(bound - counts[i], max(1, budget * weights[i] // mass), surplus)
            counts[i] = counts[i] + addition
            surplus = surplus - addition
    return np.array(counts)


def gaussian(stream_key, shape, scale, most, split=(), held_as=jnp.bfloat16):
    level = steps_of(stream_key, shape, split, -0.22, 0.18) if split else 1.0
    result = jax.random.normal(stream_key, shape, jnp.float32) * scale * level
    return jnp.minimum(jnp.maximum(result, -most), most).astype(held_as)


def setup_inputs(seed: int = 0, part: int = 0) -> dict:
    keys = jax.random.split(jax.random.key(seed), 16)
    own_keys = jax.random.split(jax.random.fold_in(keys[15], part), 16)
    mixer_input = draw_mixer_input(jax.random.fold_in(jax.random.fold_in(keys[15], part), 71), part)
    forget_cumsum = draw_forget_cumsum(jax.random.fold_in(jax.random.fold_in(keys[15], part), 71), part)
    mixer_gain = jnp.clip(1.0 + 0.18 * jax.random.normal(keys[2], (D,), jnp.float32), 0.1, 1.9)
    query_weight = draw_query_weight(jax.random.fold_in(keys[15], 71), part)
    key_weight = draw_key_weight(jax.random.fold_in(keys[15], 71), part)
    value_weight = gaussian(keys[5], (D, ATTENDER_NUMBER * HEAD_DIM), D ** -0.5, 0.125, ((1, 4),))
    out_weight = gaussian(keys[6], (ATTENDER_NUMBER * HEAD_DIM, D), (ATTENDER_NUMBER * HEAD_DIM) ** -0.5, 0.1875, ((0, 4),))
    post_gain = jnp.clip(1.0 + 0.18 * jax.random.normal(keys[7], (D,), jnp.float32), 0.1, 1.9)
    expert_input = gaussian(own_keys[8], (TOK_MOE, D), 1.0, 6.0, ((0, 16),))
    expert_gain = jnp.clip(1.0 + 0.18 * jax.random.normal(keys[9], (D,), jnp.float32), 0.1, 1.9)
    routes_keys = jax.random.split(jax.random.fold_in(own_keys[10], 1), TOK_MOE // MOE_ROWS)
    routes_turns = jax.random.permutation(jax.random.fold_in(own_keys[10], 3), TOK_MOE // MOE_ROWS)
    routes = jax.vmap(lambda own, number: shared_out(jax.random.fold_in(own_keys[10], 2), own, number, MOE_ROWS, EXPERTS, TOP, CAP, 2))(routes_keys, routes_turns).reshape((TOK_MOE, TOP))
    route_weight = jnp.clip(0.2 + 0.8 * jax.random.uniform(own_keys[11], (TOK_MOE, TOP), jnp.float32) ** steps_of(own_keys[11], (TOK_MOE, TOP), ((0, 16),), -0.2, 0.2), 0.2, 1.0)
    expert_gate = gaussian(keys[12], (EXPERTS, D, EXP_FF), D ** -0.5, 0.125, ((0, 4), (2, 4)))
    expert_upward = gaussian(keys[13], (EXPERTS, D, EXP_FF), D ** -0.5, 0.125, ((0, 4), (2, 4)))
    expert_down = gaussian(keys[14], (EXPERTS, EXP_FF, D), EXP_FF ** -0.5, 0.125, ((0, 4), (1, 4)))
    return dict(mixer_input=mixer_input, forget_cumsum=forget_cumsum, mixer_gain=mixer_gain, query_weight=query_weight, key_weight=key_weight, value_weight=value_weight, out_weight=out_weight, post_gain=post_gain, expert_input=expert_input, expert_gain=expert_gain, routes=routes, route_weight=route_weight, expert_gate=expert_gate, expert_upward=expert_upward, expert_down=expert_down)


EPS = 1e-06
MASKED = -1e+30

def normalize(rows, gain):
    values = rows.astype(jnp.float32)
    inverse = lax.rsqrt(lax.optimization_barrier(jnp.mean(values * values, axis=-1, keepdims=True)) + EPS)
    return values * inverse * gain.astype(jnp.float32)

def attend(queries, key_rows, value_rows, forget_cumsum):
    head_q = queries.reshape(WINDOW_EXTENT, ATTENDER_NUMBER, HEAD_DIM).transpose(1, 0, 2).astype(jnp.float32)
    head_k = key_rows.reshape(WINDOW_EXTENT, ATTENDER_NUMBER, HEAD_DIM).transpose(1, 0, 2).astype(jnp.float32)
    head_v = value_rows.reshape(WINDOW_EXTENT, ATTENDER_NUMBER, HEAD_DIM).transpose(1, 0, 2).astype(jnp.float32)
    block_size = math.gcd(WINDOW_EXTENT, 512)

    def one_query_block(block_index):
        first_row = block_index * block_size
        query_block = lax.dynamic_slice_in_dim(head_q, first_row, block_size, 1)
        query_gate = lax.dynamic_slice_in_dim(forget_cumsum, first_row, block_size, 1)
        query_pos = first_row + jnp.arange(block_size, dtype=jnp.int32)

        def advance_increment(key_index, state):
            running_max, running_sum, running_acc = state
            key_first = key_index * block_size
            key_block = lax.dynamic_slice_in_dim(head_k, key_first, block_size, 1)
            value_block = lax.dynamic_slice_in_dim(head_v, key_first, block_size, 1)
            key_gate = lax.dynamic_slice_in_dim(forget_cumsum, key_first, block_size, 1)
            scores = jnp.einsum('hqd,hkd->hqk', query_block, key_block) * HEAD_DIM ** (-0.5)
            scores = scores + query_gate[:, :, None] - key_gate[:, None, :]
            key_pos = key_first + jnp.arange(block_size, dtype=jnp.int32)
            visible = (key_pos[None, :] <= query_pos[:, None])[None]
            scores = jnp.where(visible, scores, MASKED)
            new_max = jnp.maximum(running_max, lax.optimization_barrier(jnp.max(scores, axis=-1)))
            weights = jnp.where(visible, jnp.exp(scores - new_max[..., None]), 0.0)
            rescale = jnp.exp(running_max - new_max)
            running_sum = running_sum * rescale + lax.optimization_barrier(jnp.sum(weights, axis=-1))
            rounded = lax.optimization_barrier(weights.astype(jnp.bfloat16)).astype(jnp.float32)
            running_acc = running_acc * rescale[..., None] + jnp.einsum('hqk,hkd->hqd', rounded, value_block)
            return (new_max, running_sum, running_acc)
        initial = (jnp.full((ATTENDER_NUMBER, block_size), MASKED, jnp.float32), jnp.zeros((ATTENDER_NUMBER, block_size), jnp.float32), jnp.zeros((ATTENDER_NUMBER, block_size, HEAD_DIM), jnp.float32))
        running_max, running_sum, running_acc = lax.fori_loop(0, block_index + 1, advance_increment, initial)
        return (running_acc / running_sum[..., None]).astype(jnp.bfloat16)
    blocks = lax.map(one_query_block, jnp.arange(WINDOW_EXTENT // block_size, dtype=jnp.int32))
    return blocks.transpose(0, 2, 1, 3).reshape(WINDOW_EXTENT, ATTENDER_NUMBER * HEAD_DIM)

def one_expert(operands):
    rows, gate_part, upward_part, down_part = operands
    group = EXP_FF // N_TP
    running = jnp.zeros((rows.shape[0], D), jnp.float32)
    for shard in range(N_TP):
        gate_proj = jnp.dot(rows, gate_part[:, shard * group:(shard + 1) * group], preferred_element_type=jnp.float32)
        upward = jnp.dot(rows, upward_part[:, shard * group:(shard + 1) * group], preferred_element_type=jnp.float32)
        hidden = (jax.nn.silu(gate_proj) * upward).astype(jnp.bfloat16)
        partial_term = jnp.dot(hidden, down_part[shard * group:(shard + 1) * group, :], preferred_element_type=jnp.float32)
        running = running + lax.optimization_barrier(partial_term.astype(jnp.bfloat16)).astype(jnp.float32)
    return running.astype(jnp.bfloat16)

def reference(mixer_input, forget_cumsum, mixer_gain, query_weight, key_weight, value_weight, out_weight, post_gain, expert_input, expert_gain, routes, route_weight, expert_gate, expert_upward, expert_down):
    normed = normalize(mixer_input, mixer_gain).astype(jnp.bfloat16)
    queries = jnp.dot(normed, query_weight, preferred_element_type=jnp.float32).astype(jnp.bfloat16)
    key_rows = jnp.dot(normed, key_weight, preferred_element_type=jnp.float32).astype(jnp.bfloat16)
    value_rows = jnp.dot(normed, value_weight, preferred_element_type=jnp.float32).astype(jnp.bfloat16)
    attended = attend(queries, key_rows, value_rows, forget_cumsum)
    group = ATTENDER_NUMBER * HEAD_DIM // N_TP
    mixer_sum = jnp.zeros((WINDOW_EXTENT, D), jnp.float32)
    for shard in range(N_TP):
        partial_term = jnp.dot(attended[:, shard * group:(shard + 1) * group], out_weight[shard * group:(shard + 1) * group, :], preferred_element_type=jnp.float32)
        mixer_sum = mixer_sum + lax.optimization_barrier(partial_term.astype(jnp.bfloat16)).astype(jnp.float32)
    mixer_output = normalize(mixer_sum, post_gain).astype(jnp.bfloat16)
    sources = N_EP * N_TP
    normed_moe = normalize(expert_input, expert_gain).astype(jnp.bfloat16)
    grouped = routes.reshape(sources, MOE_ROWS * TOP).astype(jnp.int32)
    member = (grouped[:, :, None] == jnp.arange(EXPERTS, dtype=jnp.int32)[None, None, :]).astype(jnp.int32)
    before = jnp.cumsum(member, axis=1) - member
    slot_rank = lax.optimization_barrier(jnp.sum(before * member, axis=-1))
    slot_index = grouped * (sources * CAP) + jnp.arange(sources, dtype=jnp.int32)[:, None] * CAP + slot_rank
    slot_index = slot_index.reshape(-1).astype(jnp.int32)
    repeated = jnp.repeat(normed_moe, TOP, axis=0)
    buffer = jnp.zeros((EXPERTS * sources * CAP, D), jnp.bfloat16).at[slot_index].set(repeated)
    buffer = buffer.reshape(EXPERTS, sources * CAP, D)
    outputs = lax.map(one_expert, (buffer, expert_gate, expert_upward, expert_down)).reshape(-1, D)
    picked = outputs[slot_index].reshape(TOK_MOE, TOP, D).astype(jnp.float32)
    expert_output = lax.optimization_barrier(jnp.sum(picked * route_weight.astype(jnp.float32)[:, :, None], axis=1)).astype(jnp.bfloat16)
    return (mixer_output, expert_output)
```

```python
import functools

import jax
import jax.numpy as jnp
from jax import lax
from jax.experimental import pallas as pl
from jax.experimental.pallas import tpu as pltpu
from jax.sharding import PartitionSpec as P

EPS = 1e-06
MASKED = -1e30
MESH = pl.DeviceIdType.MESH
F32 = jnp.float32
BF16 = jnp.bfloat16


def normalize(row_block, gain):
    values = row_block.astype(F32)
    inverse = lax.rsqrt(jnp.mean(values * values, axis=-1, keepdims=True) + EPS)
    return values * inverse * gain


def tile_of(width, largest):
    return largest if width % largest == 0 else width


def kernel(
    n_ep,
    head_dim,
    normed_ref,
    outgoing_ref,
    query_gate_ref,
    gate_ref,
    post_gain_ref,
    wq_hbm,
    wk_hbm,
    wv_hbm,
    wo_hbm,
    eg_hbm,
    eu_hbm,
    ed_hbm,
    mixer_ref,
    returned_ref,
    wq,
    wk,
    wv,
    wo,
    eg,
    eu,
    ed,
    seg,
    queries,
    kv,
    rows,
    hid,
    res,
    drec,
    erec,
    fin,
    run_max,
    run_sum,
    run_acc,
    attended,
    mdrec,
    merec,
    w_sem,
    ns,
    nr,
    as_,
    ar,
    bs,
    br,
    cs,
    cr,
    ds,
    dr,
    es,
    er,
    fs,
    fr,
    ks,
    kr,
    ms,
    mr,
):
    me = lax.axis_index("ep")
    t = lax.axis_index("tp")
    hi = t // 2
    lo = t % 2
    lo_peer = 2 * hi + (1 - lo)
    hi_peer = 2 * (1 - hi) + lo
    other_hi = 1 - hi
    mix_rows, width = normed_ref.shape
    head_width = wq.shape[1]
    heads = head_width // head_dim
    span = 4 * mix_rows
    cap = outgoing_ref.shape[1]

    def remote(src, dst, send_sem, recv_sem, where):
        return pltpu.make_async_remote_copy(
            src_ref=src,
            dst_ref=dst,
            send_sem=send_sem,
            recv_sem=recv_sem,
            device_id=where,
            device_id_type=MESH,
        )

    loads = [
        pltpu.make_async_copy(src, dst, w_sem.at[i])
        for i, (src, dst) in enumerate(
            ((wq_hbm, wq), (wk_hbm, wk), (wv_hbm, wv), (wo_hbm, wo), (eg_hbm, eg), (eu_hbm, eu), (ed_hbm, ed))
        )
    ]
    barrier = pltpu.get_barrier_semaphore()
    pl.semaphore_signal(barrier, inc=1, device_id={"tp": lo_peer}, device_id_type=MESH)
    pl.semaphore_signal(barrier, inc=1, device_id={"tp": hi_peer}, device_id_type=MESH)

    @pl.loop(1, n_ep)
    def _(j):
        pl.semaphore_signal(barrier, inc=1, device_id={"ep": lax.rem(me + j, n_ep)}, device_id_type=MESH)

    for load in loads:
        load.start()
    pl.semaphore_wait(barrier, 2 + n_ep - 1)

    n_hi = remote(normed_ref, seg.at[t], ns.at[0], nr.at[0], {"tp": hi_peer})
    n_lo = remote(normed_ref, seg.at[t], ns.at[1], nr.at[1], {"tp": lo_peer})
    n_relay = remote(seg.at[hi_peer], seg.at[hi_peer], ns.at[2], nr.at[2], {"tp": lo_peer})
    n_hi.start()
    n_lo.start()

    def copy_a(j):
        to = lax.rem(me - j + n_ep, n_ep)
        return remote(outgoing_ref.at[to], rows.at[j, t], as_.at[j], ar.at[j], {"ep": to})

    def copy_b_hi(j, src):
        return remote(src, rows.at[j, t], bs.at[0, j], br.at[0, j], {"tp": hi_peer})

    def copy_b_lo(j, src):
        return remote(src, rows.at[j, t], bs.at[1, j], br.at[1, j], {"tp": lo_peer})

    def copy_c(j):
        return remote(rows.at[j, hi_peer], rows.at[j, hi_peer], cs.at[j], cr.at[j], {"tp": lo_peer})

    def copy_d(j, h):
        return remote(res.at[j, 2 * h + (1 - lo)], drec.at[j, h], ds.at[h, j], dr.at[h, j], {"tp": lo_peer})

    def copy_e(j):
        return remote(drec.at[j, other_hi], erec.at[j], es.at[j], er.at[j], {"tp": hi_peer})

    def copy_f(j):
        to = lax.rem(me + j, n_ep)
        return remote(fin.at[j], returned_ref.at[me], fs.at[j], fr.at[j], {"ep": to})

    def copy_kv(b):
        return remote(kv.at[b], kv.at[b], ks.at[b], kr.at[b], {"ep": lax.rem(me + 1, n_ep)})

    @pl.loop(1, n_ep)
    def _(j):
        copy_a(j).start()

    copy_b_hi(0, outgoing_ref.at[me]).start()
    copy_b_lo(0, outgoing_ref.at[me]).start()
    seg[t] = normed_ref[...]
    rows[0, t] = outgoing_ref[me]

    n_hi.wait_recv()
    n_relay.start()
    for load in loads[:3]:
        load.wait()
    if n_ep > 1:
        copy_a(1).wait_recv()
        copy_b_hi(1, rows.at[1, t]).start()
        copy_b_lo(1, rows.at[1, t]).start()
    n_lo.wait_recv()
    n_relay.wait_recv()

    @pl.loop(0, 2)
    def _(i):
        x = seg[pl.ds(2 * i, 2)].reshape(2 * mix_rows, width)
        r = pl.ds(pl.multiple_of(i * 2 * mix_rows, 2 * mix_rows), 2 * mix_rows)
        kv[me, r, pl.ds(0, head_width)] = jnp.dot(x, wk[...], preferred_element_type=F32).astype(BF16)
        kv[me, r, pl.ds(head_width, head_width)] = jnp.dot(x, wv[...], preferred_element_type=F32).astype(BF16)
        queries[r, :] = jnp.dot(x, wq[...], preferred_element_type=F32).astype(BF16)

    @pl.when(me + 1 < n_ep)
    def _():
        copy_kv(me).start()

    copy_b_hi(0, outgoing_ref.at[me]).wait_recv()
    copy_c(0).start()
    for load in loads[4:]:
        load.wait()

    f_width = eg.shape[1]
    f_tile = tile_of(f_width, 256)
    d_tile = tile_of(width, 512)

    def step_e(j):
        copy_d(j, 0).wait_recv()
        copy_d(j, 1).wait_recv()
        drec[j, other_hi] = (res[j, hi_peer].astype(F32) + drec[j, other_hi].astype(F32)).astype(BF16)
        copy_e(j).start()

    def step_f(j):
        copy_e(j).wait_recv()
        total = (res[j, t].astype(F32) + drec[j, hi].astype(F32) + erec[j].astype(F32)).astype(BF16)

        @pl.when(j == 0)
        def _():
            returned_ref[me] = total

        @pl.when(j > 0)
        def _():
            fin[j] = total
            copy_f(j).start()

    @pl.loop(0, n_ep)
    def _(j):
        @pl.when(j + 2 < n_ep)
        def _():
            copy_a(j + 2).wait_recv()
            copy_b_hi(j + 2, rows.at[j + 2, t]).start()
            copy_b_lo(j + 2, rows.at[j + 2, t]).start()

        @pl.when(j + 1 < n_ep)
        def _():
            copy_b_hi(j + 1, rows.at[j + 1, t]).wait_recv()
            copy_c(j + 1).start()

        @pl.when((j >= 1) & (me - j >= 0))
        def _():
            copy_kv(me - j).wait_recv()

            @pl.when(me + 1 < n_ep)
            def _():
                copy_kv(me - j).start()

        copy_b_lo(j, rows.at[j, t]).wait_recv()
        copy_c(j).wait_recv()

        @pl.loop(0, f_width // f_tile)
        def _(f):
            x = rows[j].reshape(4 * cap, width)
            c = pl.ds(pl.multiple_of(f * f_tile, f_tile), f_tile)
            g = jnp.dot(x, eg[:, c], preferred_element_type=F32)
            u = jnp.dot(x, eu[:, c], preferred_element_type=F32)
            hid[:, c] = (g / (1.0 + jnp.exp(-g)) * u).astype(BF16)

        @pl.loop(0, width // d_tile)
        def _(d):
            c = pl.ds(pl.multiple_of(d * d_tile, d_tile), d_tile)
            y = jnp.dot(hid[...], ed[:, c], preferred_element_type=F32)
            res[j, :, :, c] = y.astype(BF16).reshape(4, cap, d_tile)

        copy_d(j, 0).start()
        copy_d(j, 1).start()

        @pl.when(j >= 1)
        def _():
            step_e(j - 1)

        @pl.when(j >= 2)
        def _():
            step_f(j - 2)

    step_e(n_ep - 1)
    if n_ep > 1:
        step_f(n_ep - 2)

    scale = head_dim ** (-0.5)
    q_tile = span // 2
    for h in range(heads):
        hc = pl.ds(h * head_dim, head_dim)
        vc = pl.ds(head_width + h * head_dim, head_dim)

        @pl.loop(0, 2)
        def _(i):
            r = pl.ds(pl.multiple_of(i * q_tile, q_tile), q_tile)
            run_max[...] = jnp.full_like(run_max, MASKED)
            run_sum[...] = jnp.zeros_like(run_sum)
            run_acc[...] = jnp.zeros_like(run_acc)

            def block(b, masked):
                kc = pl.ds(pl.multiple_of(b * span, span), span)
                s = lax.dot_general(
                    queries[r, hc], kv[b, :, hc], (((1,), (1,)), ((), ())), preferred_element_type=F32
                )
                s = s * scale + query_gate_ref[r, h : h + 1] - gate_ref[h : h + 1, kc]
                if masked:
                    row = lax.broadcasted_iota(jnp.int32, s.shape, 0) + i * q_tile
                    col = lax.broadcasted_iota(jnp.int32, s.shape, 1)
                    s = jnp.where(col <= row, s, MASKED)
                old = run_max[...]
                new = jnp.maximum(old, jnp.max(s, axis=1, keepdims=True))
                w = jnp.exp(s - new)
                fix = jnp.exp(old - new)
                run_max[...] = new
                run_sum[...] = run_sum[...] * fix + jnp.sum(w, axis=1, keepdims=True)
                run_acc[...] = run_acc[...] * fix + jnp.dot(
                    w.astype(BF16), kv[b, :, vc], preferred_element_type=F32
                )

            block(me, True)

            @pl.loop(0, me)
            def _(b):
                block(b, False)

            attended[r, hc] = (run_acc[...] / run_sum[...]).astype(BF16)

    loads[3].wait()
    n_relay.wait_send()
    part = seg

    def project(b):
        x = attended[pl.ds(pl.multiple_of(b * mix_rows, mix_rows), mix_rows), :]

        @pl.loop(0, width // d_tile)
        def _(d):
            c = pl.ds(pl.multiple_of(d * d_tile, d_tile), d_tile)
            part[b, :, c] = jnp.dot(x, wo[:, c], preferred_element_type=F32).astype(BF16)

    def copy_m(h):
        return remote(part.at[2 * h + (1 - lo)], mdrec.at[h], ms.at[h], mr.at[h], {"tp": lo_peer})

    m_hi = remote(mdrec.at[other_hi], merec, ms.at[2], mr.at[2], {"tp": hi_peer})
    project(2 * other_hi + (1 - lo))
    copy_m(other_hi).start()
    project(hi_peer)
    project(lo_peer)
    copy_m(hi).start()
    copy_m(other_hi).wait_recv()
    mdrec[other_hi] = (part[hi_peer].astype(F32) + mdrec[other_hi].astype(F32)).astype(BF16)
    m_hi.start()
    project(t)
    step_f(n_ep - 1)
    copy_m(hi).wait_recv()
    m_hi.wait_recv()
    total = part[t].astype(F32) + mdrec[hi].astype(F32) + merec[...].astype(F32)
    inverse = lax.rsqrt(jnp.mean(total * total, axis=-1, keepdims=True) + EPS)
    mixer_ref[...] = (total * inverse * post_gain_ref[...]).astype(BF16)

    n_hi.wait_send()
    n_lo.wait_send()
    copy_m(0).wait_send()
    copy_m(1).wait_send()
    m_hi.wait_send()

    @pl.loop(0, n_ep)
    def _(j):
        @pl.when(j > 0)
        def _():
            copy_a(j).wait_send()
            copy_f(j).wait_send()
            copy_f(j).wait_recv()

        copy_b_hi(j, rows.at[j, t]).wait_send()
        copy_b_lo(j, rows.at[j, t]).wait_send()
        copy_c(j).wait_send()
        copy_d(j, 0).wait_send()
        copy_d(j, 1).wait_send()
        copy_e(j).wait_send()

        @pl.when((j <= me) & (me + 1 < n_ep))
        def _():
            copy_kv(j).wait_send()


def on_device(
    mixer_input,
    forget_cumsum,
    mixer_gain,
    query_weight,
    key_weight,
    value_weight,
    out_weight,
    post_gain,
    expert_input,
    expert_gain,
    routes,
    route_weight,
    expert_gate,
    expert_upward,
    expert_down,
):
    n_ep = lax.axis_size("ep")
    n_tp = lax.axis_size("tp")
    mix_rows, width = mixer_input.shape
    heads = forget_cumsum.shape[0]
    head_width = query_weight.shape[1]
    head_dim = head_width // heads
    span = mix_rows * n_tp
    moe_rows, top_count = routes.shape
    experts_local = expert_gate.shape[0]
    assert n_tp == 4 and experts_local == 1
    experts_all = n_ep
    capacity = (moe_rows * top_count * 9 + 8 * experts_all - 1) // (8 * experts_all)
    cap = (capacity + ROW_TILE - 1) // ROW_TILE * ROW_TILE
    slots_all = experts_all * cap
    first_pos = lax.axis_index("ep") * span

    normed = normalize(mixer_input, mixer_gain).astype(BF16)
    normed_moe = normalize(expert_input, expert_gain).astype(BF16)
    flat_routes = routes.reshape(-1)
    member = (flat_routes[:, None] == jnp.arange(experts_all, dtype=jnp.int32)[None, :]).astype(F32)
    order = jnp.arange(moe_rows * top_count, dtype=jnp.int32)
    earlier = (order[None, :] < order[:, None]).astype(BF16)
    before = jnp.dot(earlier, member.astype(BF16), preferred_element_type=F32)
    slot_rank = jnp.sum(before * member, axis=1).astype(jnp.int32)
    slot_index = (flat_routes * cap + slot_rank).reshape(moe_rows, top_count)
    slot_ids = jnp.arange(slots_all, dtype=jnp.int32)
    choosers = [
        (slot_index[:, which][:, None] == slot_ids[None, :]).astype(BF16) for which in range(top_count)
    ]
    dispatch = functools.reduce(lambda a, b: a + b, choosers)
    outgoing = lax.dot_general(
        dispatch, normed_moe, (((0,), (0,)), ((), ())), preferred_element_type=F32
    ).astype(BF16)
    outgoing = outgoing.reshape(n_ep, cap, width)
    query_gate = lax.dynamic_slice_in_dim(forget_cumsum, first_pos, span, 1).T

    vmem = pl.BlockSpec(memory_space=pltpu.VMEM)
    hbm = pl.BlockSpec(memory_space=pl.ANY)
    dma = pltpu.SemaphoreType.DMA
    f_width = expert_gate.shape[2]
    mixer_output, returned = pl.pallas_call(
        functools.partial(kernel, n_ep, head_dim),
        out_shape=(
            jax.ShapeDtypeStruct((mix_rows, width), BF16),
            jax.ShapeDtypeStruct((n_ep, cap, width), BF16),
        ),
        in_specs=[vmem] * 5 + [hbm] * 7,
        out_specs=(vmem, vmem),
        scratch_shapes=[
            pltpu.VMEM((width, head_width), BF16),
            pltpu.VMEM((width, head_width), BF16),
            pltpu.VMEM((width, head_width), BF16),
            pltpu.VMEM((head_width, width), BF16),
            pltpu.VMEM((width, f_width), BF16),
            pltpu.VMEM((width, f_width), BF16),
            pltpu.VMEM((f_width, width), BF16),
            pltpu.VMEM((4, mix_rows, width), BF16),
            pltpu.VMEM((span, head_width), BF16),
            pltpu.VMEM((n_ep, span, 2 * head_width), BF16),
            pltpu.VMEM((n_ep, 4, cap, width), BF16),
            pltpu.VMEM((4 * cap, f_width), BF16),
            pltpu.VMEM((n_ep, 4, cap, width), BF16),
            pltpu.VMEM((n_ep, 2, cap, width), BF16),
            pltpu.VMEM((n_ep, cap, width), BF16),
            pltpu.VMEM((n_ep, cap, width), BF16),
            pltpu.VMEM((span // 2, 1), F32),
            pltpu.VMEM((span // 2, 1), F32),
            pltpu.VMEM((span // 2, head_dim), F32),
            pltpu.VMEM((span, head_width), BF16),
            pltpu.VMEM((2, mix_rows, width), BF16),
            pltpu.VMEM((mix_rows, width), BF16),
            dma((7,)),
            dma((3,)),
            dma((3,)),
            dma((n_ep,)),
            dma((n_ep,)),
            dma((2, n_ep)),
            dma((2, n_ep)),
            dma((n_ep,)),
            dma((n_ep,)),
            dma((2, n_ep)),
            dma((2, n_ep)),
            dma((n_ep,)),
            dma((n_ep,)),
            dma((n_ep,)),
            dma((n_ep,)),
            dma((n_ep,)),
            dma((n_ep,)),
            dma((3,)),
            dma((3,)),
        ],
        compiler_params=pltpu.CompilerParams(
            collective_id=0, has_side_effects=True, vmem_limit_bytes=66_500_000
        ),
    )(
        normed,
        outgoing,
        query_gate,
        forget_cumsum,
        post_gain.reshape(1, -1),
        query_weight,
        key_weight,
        value_weight,
        out_weight,
        expert_gate[0],
        expert_upward[0],
        expert_down[0],
    )
    returned = returned.reshape(slots_all, width)
    combined = jnp.zeros((moe_rows, width), F32)
    for which in range(top_count):
        picked = jnp.dot(choosers[which], returned, preferred_element_type=F32)
        combined = combined + route_weight[:, which : which + 1] * picked
    return (mixer_output, combined.astype(BF16))


ROW_TILE = 16


def solution(mesh):
    rows = P(("grp", "ep", "tp"), None)
    in_specs = (
        rows,
        P("tp", "grp"),
        P(),
        P(None, "tp"),
        P(None, "tp"),
        P(None, "tp"),
        P("tp", None),
        P(),
        rows,
        P(),
        rows,
        rows,
        P("ep", None, "tp"),
        P("ep", None, "tp"),
        P("ep", "tp", None),
    )
    return jax.shard_map(
        on_device, mesh=mesh, in_specs=in_specs, out_specs=(rows, rows), check_vma=False
    )
```

```python
import functools

import jax
import jax.numpy as jnp
from jax import lax
from jax.experimental import pallas as pl
from jax.experimental.pallas import tpu as pltpu
from jax.sharding import PartitionSpec as P

EPS = 1e-06
MASKED = -1e30
MESH = pl.DeviceIdType.MESH
F32 = jnp.float32
BF16 = jnp.bfloat16


def normalize(row_block, gain):
    values = row_block.astype(F32)
    inverse = lax.rsqrt(jnp.mean(values * values, axis=-1, keepdims=True) + EPS)
    return values * inverse * gain


def tile_of(width, largest):
    return largest if width % largest == 0 else width


def kernel(
    n_ep,
    head_dim,
    normed_ref,
    outgoing_ref,
    query_gate_ref,
    gate_ref,
    post_gain_ref,
    wq_hbm,
    wk_hbm,
    wv_hbm,
    wo_hbm,
    eg_hbm,
    eu_hbm,
    ed_hbm,
    mixer_ref,
    returned_ref,
    wq,
    wk,
    wv,
    wo,
    eg,
    eu,
    ed,
    seg,
    queries,
    kv,
    rows,
    hid,
    res,
    drec,
    erec,
    fin,
    run_max,
    run_sum,
    run_acc,
    attended,
    mdrec,
    merec,
    w_sem,
    ns,
    nr,
    as_,
    ar,
    bs,
    br,
    cs,
    cr,
    ds,
    dr,
    es,
    er,
    fs,
    fr,
    ks,
    kr,
    ms,
    mr,
):
    me = lax.axis_index("ep")
    t = lax.axis_index("tp")
    hi = t // 2
    lo = t % 2
    lo_peer = 2 * hi + (1 - lo)
    hi_peer = 2 * (1 - hi) + lo
    other_hi = 1 - hi
    mix_rows, width = normed_ref.shape
    head_width = wq.shape[1]
    heads = head_width // head_dim
    span = 4 * mix_rows
    cap = outgoing_ref.shape[1]

    def remote(src, dst, send_sem, recv_sem, where):
        return pltpu.make_async_remote_copy(
            src_ref=src,
            dst_ref=dst,
            send_sem=send_sem,
            recv_sem=recv_sem,
            device_id=where,
            device_id_type=MESH,
        )

    loads = [
        pltpu.make_async_copy(src, dst, w_sem.at[i])
        for i, (src, dst) in enumerate(
            ((wq_hbm, wq), (wk_hbm, wk), (wv_hbm, wv), (wo_hbm, wo), (eg_hbm, eg), (eu_hbm, eu), (ed_hbm, ed))
        )
    ]
    barrier = pltpu.get_barrier_semaphore()
    pl.semaphore_signal(barrier, inc=1, device_id={"tp": lo_peer}, device_id_type=MESH)
    pl.semaphore_signal(barrier, inc=1, device_id={"tp": hi_peer}, device_id_type=MESH)

    @pl.loop(1, n_ep)
    def _(j):
        pl.semaphore_signal(barrier, inc=1, device_id={"ep": lax.rem(me + j, n_ep)}, device_id_type=MESH)

    for load in loads:
        load.start()
    pl.semaphore_wait(barrier, 2 + n_ep - 1)

    n_hi = remote(normed_ref, seg.at[t], ns.at[0], nr.at[0], {"tp": hi_peer})
    n_lo = remote(normed_ref, seg.at[t], ns.at[1], nr.at[1], {"tp": lo_peer})
    n_relay = remote(seg.at[hi_peer], seg.at[hi_peer], ns.at[2], nr.at[2], {"tp": lo_peer})
    n_hi.start()
    n_lo.start()

    def copy_a(j):
        to = lax.rem(me - j + n_ep, n_ep)
        return remote(outgoing_ref.at[to], rows.at[j, t], as_.at[j], ar.at[j], {"ep": to})

    def copy_b_hi(j, src):
        return remote(src, rows.at[j, t], bs.at[0, j], br.at[0, j], {"tp": hi_peer})

    def copy_b_lo(j, src):
        return remote(src, rows.at[j, t], bs.at[1, j], br.at[1, j], {"tp": lo_peer})

    def copy_c(j):
        return remote(rows.at[j, hi_peer], rows.at[j, hi_peer], cs.at[j], cr.at[j], {"tp": lo_peer})

    def copy_d(j, h):
        return remote(res.at[j, 2 * h + (1 - lo)], drec.at[j, h], ds.at[h, j], dr.at[h, j], {"tp": lo_peer})

    def copy_e(j):
        return remote(drec.at[j, other_hi], erec.at[j], es.at[j], er.at[j], {"tp": hi_peer})

    def copy_f(j):
        to = lax.rem(me + j, n_ep)
        return remote(fin.at[j], returned_ref.at[me], fs.at[j], fr.at[j], {"ep": to})

    def copy_kv(b):
        return remote(kv.at[b], kv.at[b], ks.at[b], kr.at[b], {"ep": lax.rem(me + 1, n_ep)})

    @pl.loop(1, n_ep)
    def _(j):
        copy_a(j).start()

    copy_b_hi(0, outgoing_ref.at[me]).start()
    copy_b_lo(0, outgoing_ref.at[me]).start()
    seg[t] = normed_ref[...]
    rows[0, t] = outgoing_ref[me]

    n_hi.wait_recv()
    n_relay.start()
    for load in loads[:3]:
        load.wait()
    if n_ep > 1:
        copy_a(1).wait_recv()
        copy_b_hi(1, rows.at[1, t]).start()
        copy_b_lo(1, rows.at[1, t]).start()
    n_lo.wait_recv()
    n_relay.wait_recv()

    @pl.loop(0, 2)
    def _(i):
        x = seg[pl.ds(2 * i, 2)].reshape(2 * mix_rows, width)
        r = pl.ds(pl.multiple_of(i * 2 * mix_rows, 2 * mix_rows), 2 * mix_rows)
        kv[me, r, pl.ds(0, head_width)] = jnp.dot(x, wk[...], preferred_element_type=F32).astype(BF16)
        kv[me, r, pl.ds(head_width, head_width)] = jnp.dot(x, wv[...], preferred_element_type=F32).astype(BF16)
        queries[r, :] = jnp.dot(x, wq[...], preferred_element_type=F32).astype(BF16)

    @pl.when(me + 1 < n_ep)
    def _():
        copy_kv(me).start()

    copy_b_hi(0, outgoing_ref.at[me]).wait_recv()
    copy_c(0).start()
    for load in loads[4:]:
        load.wait()

    f_width = eg.shape[1]
    f_tile = tile_of(f_width, 256)
    d_tile = tile_of(width, 512)

    def step_e(j):
        copy_d(j, 0).wait_recv()
        copy_d(j, 1).wait_recv()
        drec[j, other_hi] = (res[j, hi_peer].astype(F32) + drec[j, other_hi].astype(F32)).astype(BF16)
        copy_e(j).start()

    def step_f(j):
        copy_e(j).wait_recv()
        total = (res[j, t].astype(F32) + drec[j, hi].astype(F32) + erec[j].astype(F32)).astype(BF16)

        @pl.when(j == 0)
        def _():
            returned_ref[me] = total

        @pl.when(j > 0)
        def _():
            fin[j] = total
            copy_f(j).start()

    @pl.loop(0, n_ep)
    def _(j):
        @pl.when(j + 2 < n_ep)
        def _():
            copy_a(j + 2).wait_recv()
            copy_b_hi(j + 2, rows.at[j + 2, t]).start()
            copy_b_lo(j + 2, rows.at[j + 2, t]).start()

        @pl.when(j + 1 < n_ep)
        def _():
            copy_b_hi(j + 1, rows.at[j + 1, t]).wait_recv()
            copy_c(j + 1).start()

        copy_b_lo(j, rows.at[j, t]).wait_recv()
        copy_c(j).wait_recv()

        @pl.loop(0, f_width // f_tile)
        def _(f):
            x = rows[j].reshape(4 * cap, width)
            c = pl.ds(pl.multiple_of(f * f_tile, f_tile), f_tile)
            g = jnp.dot(x, eg[:, c], preferred_element_type=F32)
            u = jnp.dot(x, eu[:, c], preferred_element_type=F32)
            hid[:, c] = (g / (1.0 + jnp.exp(-g)) * u).astype(BF16)

        @pl.loop(0, width // d_tile)
        def _(d):
            c = pl.ds(pl.multiple_of(d * d_tile, d_tile), d_tile)
            y = jnp.dot(hid[...], ed[:, c], preferred_element_type=F32)
            res[j, :, :, c] = y.astype(BF16).reshape(4, cap, d_tile)

        copy_d(j, 0).start()
        copy_d(j, 1).start()

        @pl.when(j >= 1)
        def _():
            step_e(j - 1)

        @pl.when((j >= 1) & (j < n_ep - 1) & (me - j >= 0))
        def _():
            copy_kv(me - j).wait_recv()

            @pl.when(me + 1 < n_ep)
            def _():
                copy_kv(me - j).start()

    step_e(n_ep - 1)

    scale = head_dim ** (-0.5)
    q_tile = span // 2
    run_max[...] = jnp.full_like(run_max, MASKED)
    run_sum[...] = jnp.zeros_like(run_sum)
    run_acc[...] = jnp.zeros_like(run_acc)

    def attend(b, masked):
        kc = pl.ds(pl.multiple_of(b * span, span), span)
        for h in range(heads):
            hc = pl.ds(h * head_dim, head_dim)
            vc = pl.ds(head_width + h * head_dim, head_dim)

            @pl.loop(0, 2)
            def _(i):
                r = pl.ds(pl.multiple_of(i * q_tile, q_tile), q_tile)
                s = lax.dot_general(
                    queries[r, hc], kv[b, :, hc], (((1,), (1,)), ((), ())), preferred_element_type=F32
                )
                s = s * scale + query_gate_ref[r, h : h + 1] - gate_ref[h : h + 1, kc]
                if masked:
                    row = lax.broadcasted_iota(jnp.int32, s.shape, 0) + i * q_tile
                    col = lax.broadcasted_iota(jnp.int32, s.shape, 1)
                    s = jnp.where(col <= row, s, MASKED)
                old = run_max[h, r]
                new = jnp.maximum(old, jnp.max(s, axis=1, keepdims=True))
                w = jnp.exp(s - new)
                fix = jnp.exp(old - new)
                run_max[h, r] = new
                run_sum[h, r] = run_sum[h, r] * fix + jnp.sum(w, axis=1, keepdims=True)
                run_acc[h, r] = run_acc[h, r] * fix + jnp.dot(
                    w.astype(BF16), kv[b, :, vc], preferred_element_type=F32
                )

    attend(me, True)
    if n_ep > 2:

        @pl.loop(0, n_ep - 2)
        def _(j):
            step_f(j)

    @pl.loop(1, me + 1)
    def _(d):
        @pl.when(d == n_ep - 1)
        def _():
            copy_kv(0).wait_recv()

        attend(me - d, False)

    for h in range(heads):
        attended[:, pl.ds(h * head_dim, head_dim)] = (run_acc[h] / run_sum[h]).astype(BF16)
    if n_ep > 1:
        step_f(n_ep - 2)

    loads[3].wait()
    n_relay.wait_send()
    part = seg

    def project(b):
        x = attended[pl.ds(pl.multiple_of(b * mix_rows, mix_rows), mix_rows), :]

        @pl.loop(0, width // d_tile)
        def _(d):
            c = pl.ds(pl.multiple_of(d * d_tile, d_tile), d_tile)
            part[b, :, c] = jnp.dot(x, wo[:, c], preferred_element_type=F32).astype(BF16)

    def copy_m(h):
        return remote(part.at[2 * h + (1 - lo)], mdrec.at[h], ms.at[h], mr.at[h], {"tp": lo_peer})

    m_hi = remote(mdrec.at[other_hi], merec, ms.at[2], mr.at[2], {"tp": hi_peer})
    project(2 * other_hi + (1 - lo))
    copy_m(other_hi).start()
    project(hi_peer)
    project(lo_peer)
    copy_m(hi).start()
    copy_m(other_hi).wait_recv()
    mdrec[other_hi] = (part[hi_peer].astype(F32) + mdrec[other_hi].astype(F32)).astype(BF16)
    m_hi.start()
    project(t)
    step_f(n_ep - 1)
    copy_m(hi).wait_recv()
    m_hi.wait_recv()
    total = part[t].astype(F32) + mdrec[hi].astype(F32) + merec[...].astype(F32)
    inverse = lax.rsqrt(jnp.mean(total * total, axis=-1, keepdims=True) + EPS)
    mixer_ref[...] = (total * inverse * post_gain_ref[...]).astype(BF16)

    n_hi.wait_send()
    n_lo.wait_send()
    copy_m(0).wait_send()
    copy_m(1).wait_send()
    m_hi.wait_send()

    @pl.loop(0, n_ep)
    def _(j):
        @pl.when(j > 0)
        def _():
            copy_a(j).wait_send()
            copy_f(j).wait_send()
            copy_f(j).wait_recv()

        copy_b_hi(j, rows.at[j, t]).wait_send()
        copy_b_lo(j, rows.at[j, t]).wait_send()
        copy_c(j).wait_send()
        copy_d(j, 0).wait_send()
        copy_d(j, 1).wait_send()
        copy_e(j).wait_send()

        @pl.when((j <= me) & (me + 1 < n_ep))
        def _():
            copy_kv(j).wait_send()


def on_device(
    mixer_input,
    forget_cumsum,
    mixer_gain,
    query_weight,
    key_weight,
    value_weight,
    out_weight,
    post_gain,
    expert_input,
    expert_gain,
    routes,
    route_weight,
    expert_gate,
    expert_upward,
    expert_down,
):
    n_ep = lax.axis_size("ep")
    n_tp = lax.axis_size("tp")
    mix_rows, width = mixer_input.shape
    heads = forget_cumsum.shape[0]
    head_width = query_weight.shape[1]
    head_dim = head_width // heads
    span = mix_rows * n_tp
    moe_rows, top_count = routes.shape
    experts_local = expert_gate.shape[0]
    assert n_tp == 4 and experts_local == 1
    experts_all = n_ep
    capacity = (moe_rows * top_count * 9 + 8 * experts_all - 1) // (8 * experts_all)
    cap = (capacity + ROW_TILE - 1) // ROW_TILE * ROW_TILE
    slots_all = experts_all * cap
    first_pos = lax.axis_index("ep") * span

    normed = normalize(mixer_input, mixer_gain).astype(BF16)
    normed_moe = normalize(expert_input, expert_gain).astype(BF16)
    flat_routes = routes.reshape(-1)
    member = (flat_routes[:, None] == jnp.arange(experts_all, dtype=jnp.int32)[None, :]).astype(F32)
    order = jnp.arange(moe_rows * top_count, dtype=jnp.int32)
    earlier = (order[None, :] < order[:, None]).astype(BF16)
    before = jnp.dot(earlier, member.astype(BF16), preferred_element_type=F32)
    slot_rank = jnp.sum(before * member, axis=1).astype(jnp.int32)
    slot_index = (flat_routes * cap + slot_rank).reshape(moe_rows, top_count)
    slot_ids = jnp.arange(slots_all, dtype=jnp.int32)
    choosers = [
        (slot_index[:, which][:, None] == slot_ids[None, :]).astype(BF16) for which in range(top_count)
    ]
    dispatch = functools.reduce(lambda a, b: a + b, choosers)
    outgoing = lax.dot_general(
        dispatch, normed_moe, (((0,), (0,)), ((), ())), preferred_element_type=F32
    ).astype(BF16)
    outgoing = outgoing.reshape(n_ep, cap, width)
    query_gate = lax.dynamic_slice_in_dim(forget_cumsum, first_pos, span, 1).T

    vmem = pl.BlockSpec(memory_space=pltpu.VMEM)
    hbm = pl.BlockSpec(memory_space=pl.ANY)
    dma = pltpu.SemaphoreType.DMA
    f_width = expert_gate.shape[2]
    mixer_output, returned = pl.pallas_call(
        functools.partial(kernel, n_ep, head_dim),
        out_shape=(
            jax.ShapeDtypeStruct((mix_rows, width), BF16),
            jax.ShapeDtypeStruct((n_ep, cap, width), BF16),
        ),
        in_specs=[vmem] * 5 + [hbm] * 7,
        out_specs=(vmem, vmem),
        scratch_shapes=[
            pltpu.VMEM((width, head_width), BF16),
            pltpu.VMEM((width, head_width), BF16),
            pltpu.VMEM((width, head_width), BF16),
            pltpu.VMEM((head_width, width), BF16),
            pltpu.VMEM((width, f_width), BF16),
            pltpu.VMEM((width, f_width), BF16),
            pltpu.VMEM((f_width, width), BF16),
            pltpu.VMEM((4, mix_rows, width), BF16),
            pltpu.VMEM((span, head_width), BF16),
            pltpu.VMEM((n_ep, span, 2 * head_width), BF16),
            pltpu.VMEM((n_ep, 4, cap, width), BF16),
            pltpu.VMEM((4 * cap, f_width), BF16),
            pltpu.VMEM((n_ep, 4, cap, width), BF16),
            pltpu.VMEM((n_ep, 2, cap, width), BF16),
            pltpu.VMEM((n_ep, cap, width), BF16),
            pltpu.VMEM((n_ep, cap, width), BF16),
            pltpu.VMEM((heads, span, 1), F32),
            pltpu.VMEM((heads, span, 1), F32),
            pltpu.VMEM((heads, span, head_dim), F32),
            pltpu.VMEM((span, head_width), BF16),
            pltpu.VMEM((2, mix_rows, width), BF16),
            pltpu.VMEM((mix_rows, width), BF16),
            dma((7,)),
            dma((3,)),
            dma((3,)),
            dma((n_ep,)),
            dma((n_ep,)),
            dma((2, n_ep)),
            dma((2, n_ep)),
            dma((n_ep,)),
            dma((n_ep,)),
            dma((2, n_ep)),
            dma((2, n_ep)),
            dma((n_ep,)),
            dma((n_ep,)),
            dma((n_ep,)),
            dma((n_ep,)),
            dma((n_ep,)),
            dma((n_ep,)),
            dma((3,)),
            dma((3,)),
        ],
        compiler_params=pltpu.CompilerParams(
            collective_id=0, has_side_effects=True, vmem_limit_bytes=66_500_000
        ),
    )(
        normed,
        outgoing,
        query_gate,
        forget_cumsum,
        post_gain.reshape(1, -1),
        query_weight,
        key_weight,
        value_weight,
        out_weight,
        expert_gate[0],
        expert_upward[0],
        expert_down[0],
    )
    returned = returned.reshape(slots_all, width)
    combined = jnp.zeros((moe_rows, width), F32)
    for which in range(top_count):
        picked = jnp.dot(choosers[which], returned, preferred_element_type=F32)
        combined = combined + route_weight[:, which : which + 1] * picked
    return (mixer_output, combined.astype(BF16))


ROW_TILE = 8


def solution(mesh):
    rows = P(("grp", "ep", "tp"), None)
    in_specs = (
        rows,
        P("tp", "grp"),
        P(),
        P(None, "tp"),
        P(None, "tp"),
        P(None, "tp"),
        P("tp", None),
        P(),
        rows,
        P(),
        rows,
        rows,
        P("ep", None, "tp"),
        P("ep", None, "tp"),
        P("ep", "tp", None),
    )
    return jax.shard_map(
        on_device, mesh=mesh, in_specs=in_specs, out_specs=(rows, rows), check_vma=False
    )
```
